256 devices in a mesh: dp: 4 (over x), kv: 32 (over z, y), tp: 2 (over core).
Axes of the slice: x: 4, y: 4, z: 8, core: 2. Of those that a mesh axis runs over, the one named last changes fastest.
Arguments:
- tokens: bfloat16 [512, 2048], P('dp', ('kv', 'tp')), may hold values from -30 to 30
- state: float32 [512, 4, 256, 512], P(('dp', 'kv'), 'tp'), may hold values from -6 to 6
- mix_gain: float32 [2048], P('kv'), may hold values from 0.1 to 1.9
- w_query: bfloat16 [2048, 1024], P('kv', 'tp'), may hold values from -0.125 to 0.125
- w_key: bfloat16 [2048, 1024], P('kv', 'tp'), may hold values from -0.125 to 0.125
- w_decay: bfloat16 [2048, 1024], P('kv', 'tp'), may hold values from -0.125 to 0.125
- w_value: bfloat16 [2048, 2048], P('kv', 'tp'), may hold values from -0.125 to 0.125
- w_gate: bfloat16 [2048, 2048], P('kv', 'tp'), may hold values from -0.125 to 0.125
- decay_offset: float32 [1024], P('tp'), may hold values from -1 to 4
- head_gain: float32 [512], replicated, may hold values from 0.1 to 1.9
- w_out: bfloat16 [2048, 2048], P('tp', 'kv'), may hold values from -0.125 to 0.125
- mlp_gain: float32 [2048], replicated, may hold values from 0.1 to 1.9
- w_up: bfloat16 [2048, 8192], P(None, ('kv', 'tp')), may hold values from -0.125 to 0.125
- w_down: bfloat16 [8192, 2048], P(('kv', 'tp')), may hold values from -0.1875 to 0.1875
Outputs:
- mixed: bfloat16 [512, 2048], P('dp', ('kv', 'tp'))
- new_state: float32 [512, 4, 256, 512], P(('dp', 'kv'), 'tp')
The draws below stay inside these ranges and needn't reach their ends.
All inputs are finite; a program needn't handle non-finite values.
Results may differ from the reference program's by a relative error of at most 0.013.
Values may be sent and summed in bfloat16 or wider, within the bound.
A program may use at most 64 MiB of HBM per device.

```python
import math
import jax
import jax.numpy as jnp
from jax import lax

D = 2048
HEADS = 4
KEY_DIM = 256
VAL_DIM = 512
FF = 8192
BATCH = 512


def draw_tokens(key, part):
    base_key, row_key = jax.random.split(key)
    columns = jnp.exp(jnp.linspace(math.log(0.4), math.log(2.4), D)).astype(jnp.float32)
    base = jnp.clip(jax.random.normal(base_key, (BATCH, D), jnp.float32), -6.0, 6.0)
    rowwise = jnp.exp(jax.random.uniform(row_key, (BATCH,), jnp.float32, math.log(0.5), math.log(2.0)))
    return (base * rowwise[:, None] * columns[None, :]).astype(jnp.bfloat16)


def strengthened(entries, key, source, target, blocks, factor):
    owner, partner = [(jnp.arange(entries.shape[dim]) // (entries.shape[dim] // blocks)).reshape([-1 if axis == dim else 1 for axis in range(entries.ndim)]) for dim in (source, target)]
    chosen = jax.random.permutation(key, blocks)[partner]
    strong = (owner == chosen) | (owner == (partner + blocks // 2) % blocks)
    return jnp.where(strong, factor * entries, entries)


def shard_levels(key, shape, shards, smallest, largest):
    factor_of = 1.0
    for axis_at, parts in shards:
        heights = jax.random.uniform(jax.random.fold_in(jax.random.fold_in(key, 6), axis_at), (parts,), jnp.float32, smallest / len(shards), largest / len(shards))
        factor_of = factor_of * jnp.repeat(jnp.exp(heights), shape[axis_at] // parts).reshape((-1,) + (1,) * (len(shape) - 1 - axis_at))
    return factor_of


def centred(stream_key, dims, scale, most, shards=(), kind=jnp.bfloat16):
    array = jax.random.normal(stream_key, dims, jnp.float32) * scale
    if len(shards) > 0:
        array = shard_levels(stream_key, dims, shards, -0.22, 0.18) * array
    return jnp.clip(array, min=-most, max=most).astype(kind)


def heavy_noise(rng, extent, scale, limit, cuts, heavy, held_as=jnp.bfloat16):
    entries = scale * jax.random.normal(rng, extent, jnp.float32)
    if cuts:
        entries = entries * shard_levels(rng, extent, cuts, -0.22, 0.18)
    return jnp.clip(strengthened(entries, jax.random.fold_in(rng, 3), *heavy), -limit, limit).astype(held_as)


def setup_inputs(seed: int = 0) -> dict:
    key_list = jax.random.split(jax.random.key(seed), 15)
    return {
        "tokens": draw_tokens(jax.random.fold_in(key_list[14], 71), 0),
        "state": centred(key_list[1], (BATCH, HEADS, KEY_DIM, VAL_DIM), 1.0, 6.0, ((0, 128), (1, 2)), jnp.float32),
        "mix_gain": jnp.clip(1.0 + 0.18 * jax.random.normal(key_list[2], (D,), jnp.float32), 0.1, 1.9),
        "w_query": centred(key_list[3], (D, HEADS * KEY_DIM), D ** -0.5, 0.125, ((0, 32), (1, 2))),
        "w_key": centred(key_list[4], (D, HEADS * KEY_DIM), D ** -0.5, 0.125, ((0, 32), (1, 2))),
        "w_decay": centred(key_list[5], (D, HEADS * KEY_DIM), D ** -0.5, 0.125, ((0, 32), (1, 2))),
        "w_value": centred(key_list[6], (D, HEADS * VAL_DIM), D ** -0.5, 0.125, ((0, 32), (1, 2))),
        "w_gate": centred(key_list[7], (D, HEADS * VAL_DIM), D ** -0.5, 0.125, ((0, 32), (1, 2))),
        "decay_offset": jnp.clip(-1.0 + 5.0 * jax.random.uniform(key_list[8], (HEADS * KEY_DIM,), jnp.float32) ** shard_levels(key_list[8], (HEADS * KEY_DIM,), ((0, 2),), -0.2, 0.2), -1.0, 4.0),
        "head_gain": jnp.clip(1.0 + 0.18 * jax.random.normal(key_list[9], (VAL_DIM,), jnp.float32), 0.1, 1.9),
        "w_out": centred(key_list[10], (HEADS * VAL_DIM, D), (HEADS * VAL_DIM) ** -0.5, 0.125, ((0, 2), (1, 32))),
        "mlp_gain": jnp.clip(1.0 + 0.18 * jax.random.normal(key_list[11], (D,), jnp.float32), 0.1, 1.9),
        "w_up": centred(key_list[12], (D, FF), D ** -0.5, 0.125, ((1, 64),)),
        "w_down": heavy_noise(key_list[13], (FF, D), FF ** -0.5, 0.1875, ((0, 64),), (0, 1, 64, 4.0)),
    }


epsilon = 1e-06

def reference(tokens, state, mix_gain, w_query, w_key, w_decay, w_value, w_gate, decay_offset, head_gain, w_out, mlp_gain, w_up, w_down):
    tok_float = tokens.astype(jnp.float32)
    row_scale = lax.rsqrt(lax.optimization_barrier(jnp.mean(tok_float * tok_float, axis=1, keepdims=True)) + epsilon)
    scaled = (tok_float * mix_gain).astype(jnp.bfloat16)

    def project(weight):
        return jnp.dot(scaled, weight, preferred_element_type=jnp.float32) * row_scale
    queries = (project(w_query) * KEY_DIM ** (-0.5)).reshape(BATCH, HEADS, KEY_DIM)
    new_keys = project(w_key).reshape(BATCH, HEADS, KEY_DIM)
    values = project(w_value).reshape(BATCH, HEADS, VAL_DIM)
    gates = project(w_gate)
    retain = jax.nn.sigmoid(project(w_decay) + decay_offset).reshape(BATCH, HEADS, KEY_DIM)
    new_state = retain[..., None] * state + new_keys[..., None] * values[:, :, None, :]
    readout = jnp.einsum('bhk,bhkv->bhv', queries, new_state, precision=lax.Precision.HIGHEST)
    readout = readout * lax.rsqrt(lax.optimization_barrier(jnp.mean(readout * readout, axis=2, keepdims=True)) + epsilon) * head_gain
    gated = (readout.reshape(BATCH, HEADS * VAL_DIM) * jax.nn.silu(gates)).astype(jnp.bfloat16)
    stream = (tok_float + jnp.dot(gated, w_out, preferred_element_type=jnp.float32)).astype(jnp.bfloat16)
    stream_float = stream.astype(jnp.float32)
    mlp_scale = lax.rsqrt(lax.optimization_barrier(jnp.mean(stream_float * stream_float, axis=1, keepdims=True)) + epsilon)
    normed = (stream_float * mlp_gain).astype(jnp.bfloat16)
    hidden = jnp.dot(normed, w_up, preferred_element_type=jnp.float32) * mlp_scale
    squared = jnp.square(jax.nn.relu(hidden)).astype(jnp.bfloat16)
    mixed = (stream_float + jnp.dot(squared, w_down, preferred_element_type=jnp.float32)).astype(jnp.bfloat16)
    return (mixed, new_state)
```

```python
import jax
import jax.numpy as jnp
from jax import lax
from jax.experimental import pallas as pl
from jax.experimental.pallas import tpu as pltpu
from jax.sharding import PartitionSpec as P

MESH = pl.DeviceIdType.MESH
F32, BF16 = jnp.float32, jnp.bfloat16
D = 2048
EPS = 1e-06
NY, NZ = 4, 8
Q, K, R, S, V, G = (slice(0, 128), slice(128, 256), slice(256, 384), slice(384, 512), slice(512, 768), slice(768, 1024))
PIECES = ((V, (3,)), (G, (4,)), (slice(0, 256), (0, 1)), (slice(256, 512), (2,)))
COLUMNS = (Q, K, R, V, G)


def halves_side_by_side(top, bottom):
    lane = lax.broadcasted_iota(jnp.int32, top.shape, 1)
    return jnp.where(lane < 64, top, pltpu.roll(bottom, 64, 1))


def second_halves(top, bottom):
    lane = lax.broadcasted_iota(jnp.int32, top.shape, 1)
    return jnp.where(lane < 64, pltpu.roll(top, 64, 1), bottom)


def step(
    tok_h, state_h, gain_h, wq_h, wk_h, wd_h, wv_h, wg_h, off_h, hg_h, wo_h, mg_h, wu_h, wdn_h,
    mixed_ref, new_h,
    toks, pad, unit, gain, wq, wk, wd, wv, wg, off, hg, mg, wo, wu, wdn, state,
    xg, wgat, zs, zr, ys, yr, cols, vals, gs, gr, gf, sp, sr, xf, fs, fr, fz, zr6, mx,
    send_sem, recv_sem, local_sem, gr_sem,
):
    kv, t = lax.axis_index("kv"), lax.axis_index("tp")
    y, z = lax.rem(kv, NY), lax.div(kv, NY)
    other = 1 - t

    def at_y(dy):
        return lax.rem(y + dy + NY, NY)

    def at_z(dz):
        return lax.rem(z + dz + NZ, NZ)

    barrier = pltpu.get_barrier_semaphore()

    def greet(to_y, to_z, to_t):
        pl.semaphore_signal(
            barrier, inc=1, device_id={"kv": to_z * NY + to_y, "tp": to_t}, device_id_type=MESH
        )

    greet(y, z, other)
    for dy in range(1, NY):
        greet(at_y(dy), z, t)
        greet(at_y(dy), z, other)
    for dz in range(1, NZ):
        greet(y, at_z(dz), t)
        greet(y, at_z(dz), other)
    greetings = 1 + 2 * (NY - 1) + 2 * (NZ - 1)

    local = []

    def fetch(src, dst):
        copy = pltpu.make_async_copy(src, dst, local_sem.at[len(local)])
        copy.start()
        local.append(copy)
        return copy

    sends = []

    def send(src, dst, to_y, to_z, to_t, recv=None):
        n = len(sends)
        copy = pltpu.make_async_remote_copy(
            src_ref=src,
            dst_ref=dst,
            send_sem=send_sem.at[n],
            recv_sem=recv_sem.at[n] if recv is None else recv,
            device_id={"kv": to_z * NY + to_y, "tp": to_t},
            device_id_type=MESH,
        )
        copy.start()
        sends.append(copy)
        return copy

    tok_in = [fetch(tok_h, toks.at[t]), fetch(gain_h, gain)]
    weights, staged = (wq_h, wk_h, wd_h, wv_h, wg_h), (wq, wk, wd, wv, wg)
    weight_in, own_in = [None] * 5, [None] * 5
    for n in (3, 4, 0, 1, 2):
        weight_in[n] = fetch(weights[n], staged[n])
    for n in (3, 4, 0, 1, 2):
        width = COLUMNS[n].stop - COLUMNS[n].start
        mine = pl.ds(pl.multiple_of(y * width, width), width)
        own_in[n] = fetch(
            weights[n].at[:, mine], wgat.at[pl.ds(pl.multiple_of(y * 64, 64), 64), COLUMNS[n]]
        )
    half_lanes = pl.ds(pl.multiple_of(t * 128, 128), 128)
    half_rows = pl.ds(pl.multiple_of(t * 128, 128), 128)
    wo_in = fetch(wo_h, wo.at[t])
    wu_in = fetch(wu_h, wu.at[:, half_lanes])
    wdn_in = fetch(wdn_h, wdn.at[half_rows])
    small_in = [fetch(off_h, off), fetch(hg_h, hg), fetch(mg_h, mg)]
    state_in = fetch(state_h, state)

    for copy in tok_in:
        copy.wait()
    tok = toks[t].astype(F32)
    both_gains = gain[...]
    my_gain = jnp.where(t == 0, both_gains[:, :32], both_gains[:, 32:])
    pad[...] = jnp.zeros_like(pad)
    pad[:, 0:32] = (tok * my_gain).astype(BF16).astype(F32)
    pad[:, 32:64] = tok
    turned = pad[...].T
    squares = jnp.sum(turned[32:64] * turned[32:64], axis=0, keepdims=True)
    high = squares.astype(BF16).astype(F32)
    rows = lax.broadcasted_iota(jnp.int32, (16, 128), 0)
    sums = jnp.where(rows == 0, high, jnp.where(rows == 1, squares - high, 0.0))
    unit[0:32] = turned[0:32].astype(BF16)
    unit[32:48] = sums.astype(BF16)
    xg[y, t] = unit[...]
    for copy in weight_in:
        copy.wait()

    pl.semaphore_wait(barrier, greetings)

    x_in = [send(unit, xg.at[y, t], y, z, other)]
    for dy in range(1, NY):
        x_in.append(send(unit, xg.at[y, t], at_y(dy), z, t))
        x_in.append(send(unit, xg.at[y, t], at_y(dy), z, other))
    w_in = [[] for _ in range(5)]
    for n in (3, 4, 0, 1, 2):
        width = COLUMNS[n].stop - COLUMNS[n].start
        for dy in (2, 1, 3):
            theirs = pl.ds(pl.multiple_of(at_y(dy) * width, width), width)
            w_in[n].append(
                send(
                    staged[n].at[:, theirs],
                    wgat.at[pl.ds(pl.multiple_of(y * 64, 64), 64), COLUMNS[n]],
                    at_y(dy),
                    z,
                    t,
                )
            )
    wo_in.wait()
    wu_in.wait()
    wdn_in.wait()
    twin_in = [
        send(toks.at[t], toks.at[t], y, z, other),
        send(wo.at[t], wo.at[t], y, z, other),
        send(wu.at[:, half_lanes], wu.at[:, half_lanes], y, z, other),
        send(wdn.at[half_rows], wdn.at[half_rows], y, z, other),
    ]

    for copy in x_in:
        copy.wait_recv()
    blocks = [xg[a, b].astype(F32) for a in range(NY) for b in range(2)]
    x = jnp.concatenate([block[0:32] for block in blocks], axis=0).T.astype(BF16)
    row_squares = sum(block[32:33] + block[33:34] for block in blocks)
    spread = jnp.broadcast_to(row_squares, (128, 128)).T
    spread_high = spread.astype(BF16).astype(F32)
    lane = lax.broadcasted_iota(jnp.int32, (128, 128), 1)
    zs[:, S] = jnp.where(lane < 64, spread_high, spread - spread_high).astype(BF16)
    z_in = []
    for columns, members in PIECES:
        for n in members:
            own_in[n].wait()
            for copy in w_in[n]:
                copy.wait_recv()
        if members == (2,):
            zs[:, R] = jnp.dot(x, wgat[:, R], preferred_element_type=F32).astype(BF16)
        else:
            zs[:, columns] = jnp.dot(x, wgat[:, columns], preferred_element_type=F32).astype(BF16)
        z_in.append([])
        for dz in (4, 3, 5, 2, 6, 1, 7):
            theirs = pl.ds(pl.multiple_of(at_z(dz) * 16, 16), 16)
            z_in[-1].append(
                send(zs.at[theirs, columns], zr.at[z, :, columns], y, at_z(dz), t)
            )
    for (columns, members), copies in zip(PIECES, z_in):
        mine = pl.ds(pl.multiple_of(z * 16, 16), 16)
        total = zs[mine, columns].astype(F32)
        for copy in copies:
            copy.wait_recv()
        for dz in range(1, NZ):
            total = total + zr[at_z(dz), :, columns].astype(F32)
        for a in range(NY):
            ys[a, :, columns] = total[4 * a : 4 * a + 4]
    y_in = [send(ys.at[at_y(dy)], yr.at[y], at_y(dy), z, t) for dy in (2, 1, 3)]
    yr[y] = ys[y]
    for copy in small_in:
        copy.wait()
    state_in.wait()
    for copy in y_in:
        copy.wait_recv()

    got = [yr[a] for a in range(NY)]
    row_sum = got[0][:, 384:385] + got[0][:, 448:449]
    scale = lax.rsqrt(row_sum / D + EPS)
    queries = jnp.concatenate([g[:, Q] for g in got], axis=1) * scale * (256 ** -0.5)
    keys = jnp.concatenate([g[:, K] for g in got], axis=1) * scale
    retain = jax.nn.sigmoid(jnp.concatenate([g[:, R] for g in got], axis=1) * scale + off[...])
    cols[0:4] = queries
    cols[4:8] = keys
    cols[8:12] = retain
    cols[12:16] = jnp.zeros((4, 512), F32)
    upright = cols[...].T
    values = jnp.concatenate([g[:, V] for g in got], axis=1) * scale
    gates = jnp.concatenate([g[:, G] for g in got], axis=1) * scale
    silu = gates * jax.nn.sigmoid(gates)
    new_out = []
    for b in range(4):
        for h in range(2):
            value = values[b : b + 1, h * 512 : h * 512 + 512]
            total = jnp.zeros((8, 512), F32)
            for i in range(0, 256, 32):
                at = slice(h * 256 + i, h * 256 + i + 32)
                fresh = (
                    upright[at, 8 + b : 9 + b] * state[b, h, i : i + 32, :]
                    + upright[at, 4 + b : 5 + b] * value
                )
                state[b, h, i : i + 32, :] = fresh
                part = upright[at, b : b + 1] * fresh
                total = total + ((part[0:8] + part[8:16]) + (part[16:24] + part[24:32]))
            readout = jnp.sum(total, axis=0, keepdims=True)
            power = jnp.mean(readout * readout, axis=1, keepdims=True)
            vals[b : b + 1, h * 512 : h * 512 + 512] = (
                readout * lax.rsqrt(power + EPS) * hg[...]
            )
    gs[...] = (vals[...] * silu).astype(BF16)
    for b in range(4):
        new_out.append(fetch(state.at[b], new_h.at[b]))

    low = lax.rem(z, 4)
    home = lax.div(z, 4)
    for dz in range(1, NZ):
        send(gs, gr.at[y, low, t], y, at_z(dz), home, gr_sem.at[low, t])
    n = len(sends)

    @pl.when(home != t)
    def _():
        pltpu.make_async_remote_copy(
            src_ref=gs, dst_ref=gr.at[y, low, t], send_sem=send_sem.at[n], recv_sem=gr_sem.at[low, t],
            device_id={"kv": kv, "tp": other}, device_id_type=MESH,
        ).start()

    @pl.when(home == t)
    def _():
        gr[y, low, t] = gs[...]

    twin_gs = pltpu.make_async_copy(gs, gs, send_sem.at[n])
    sends.append(None)
    g_in = []
    for a in range(4):
        for c in range(2):
            @pl.when(jnp.logical_or(z != 4 * t + a, t != c))
            def _():
                pltpu.make_async_copy(gs, gr.at[y, a, c], gr_sem.at[a, c]).wait()
        g_in.append([send(gr.at[y, a], gr.at[y, a], at_y(dy), z, t) for dy in (2, 1, 3)])
    for copies in g_in:
        for copy in copies:
            copy.wait_recv()
    for a in range(4):
        for yy in range(NY):
            for c in range(2):
                gf[16 * a + 4 * yy : 16 * a + 4 * yy + 4, 1024 * c : 1024 * c + 1024] = gr[yy, a, c].astype(F32)

    for copy in twin_in:
        copy.wait_recv()
    branch = jnp.dot(gf[:, 0:1024].astype(BF16), wo[0], preferred_element_type=F32) + jnp.dot(
        gf[:, 1024:2048].astype(BF16), wo[1], preferred_element_type=F32
    )
    here = pl.ds(pl.multiple_of(t * 64, 64), 64)
    own_tok = jnp.concatenate([toks[0, here, :].astype(F32), toks[1, here, :].astype(F32)], axis=1)
    stream = (own_tok + branch).astype(BF16).astype(F32)
    packed = jnp.concatenate([stream[0:32], stream[32:64]], axis=1)
    sp[...] = packed.astype(BF16)
    s_in = {}
    for dz in (4, 3, 5, 2, 6, 1, 7):
        s_in[dz] = send(sp, sr.at[z, y], y, at_z(dz), t)
    sr[z, y] = sp[...]
    s_y = {}
    for dz in (0, 1, 7, 2, 6, 3, 5, 4):
        if dz:
            s_in[dz].wait_recv()
        src = at_z(-dz)
        s_y[dz] = [send(sr.at[src, y], sr.at[src, y], at_y(dy), z, t) for dy in (2, 1, 3)]
    hidden = jnp.zeros((64, 256), F32)
    power = jnp.zeros((64, 256), F32)
    for dz in (0, 1, 7, 2, 6, 3, 5, 4):
        src = at_z(-dz)
        for copy in s_y[dz]:
            copy.wait_recv()
        for p in range(2):
            a, b = sr[src, 2 * p].astype(F32), sr[src, 2 * p + 1].astype(F32)
            xf[0:32, 128 * p : 128 * p + 128] = halves_side_by_side(a, b)
            xf[32:64, 128 * p : 128 * p + 128] = second_halves(a, b)
        block = xf[...]
        power = power + block * block
        gain_here = mg[:, pl.ds(pl.multiple_of(src * 256, 256), 256)]
        hidden = hidden + jnp.dot(
            (block * gain_here).astype(BF16),
            wu[pl.ds(pl.multiple_of(src * 256, 256), 256), :],
            preferred_element_type=F32,
        )
    mlp_scale = lax.rsqrt(jnp.sum(power, axis=1, keepdims=True) / D + EPS)
    squared = jnp.square(jnp.maximum(hidden * mlp_scale, 0.0)).astype(BF16)

    order = (4, 3, 5, 2, 6, 1, 7, 0)
    d_in = {}
    for dz in order:
        theirs = pl.ds(pl.multiple_of(at_z(dz) * 256, 256), 256)
        part = jnp.dot(squared, wdn[:, theirs], preferred_element_type=F32)
        for p in range(2):
            top, bottom = part[0:32, 128 * p : 128 * p + 128], part[32:64, 128 * p : 128 * p + 128]
            fs[dz, 2 * p] = halves_side_by_side(top, bottom).astype(BF16)
            fs[dz, 2 * p + 1] = second_halves(top, bottom).astype(BF16)
        d_in[dz] = [send(fs.at[dz, at_y(dy)], fr.at[dz, dy], at_y(dy), z, t) for dy in (2, 1, 3)]
    e_in = []
    for dz in order:
        for copy in d_in[dz]:
            copy.wait_recv()
        total = fs[dz, y].astype(F32)
        for dy in range(1, NY):
            total = total + fr[dz, dy].astype(F32)
        if dz:
            fz[dz] = total.astype(BF16)
            e_in.append(send(fz.at[dz], zr6.at[dz], y, at_z(dz), t))
    for copy in e_in:
        copy.wait_recv()
    for dz in range(1, NZ):
        total = total + zr6[dz].astype(F32)
    mx[t] = (packed + total).astype(BF16)
    m_in = send(mx.at[t], mx.at[t], y, z, other)
    m_in.wait_recv()
    for c in range(2):
        block = mx[c].astype(F32)
        for h in range(2):
            quarter = jnp.where(
                t == 0, block[:, h * 64 : h * 64 + 32], block[:, h * 64 + 32 : h * 64 + 64]
            )
            mixed_ref[c * 64 + h * 32 : c * 64 + h * 32 + 32, :] = quarter.astype(BF16)

    for copy in sends:
        if copy is not None:
            copy.wait_send()

    @pl.when(home != t)
    def _():
        twin_gs.wait()

    for copy in new_out:
        copy.wait()


SENDS = 7 + 15 + 4 + 28 + 3 + 8 + 12 + 7 + 24 + 24 + 7 + 1


def shards(tokens, state, mix_gain, w_query, w_key, w_decay, w_value, w_gate, decay_offset, head_gain, w_out, mlp_gain, w_up, w_down):
    anywhere = pl.BlockSpec(memory_space=pl.ANY)
    vmem = pltpu.VMEM
    mixed, new_state = pl.pallas_call(
        step,
        out_shape=(
            jax.ShapeDtypeStruct(tokens.shape, BF16),
            jax.ShapeDtypeStruct(state.shape, F32),
        ),
        in_specs=[anywhere] * 14,
        out_specs=(pl.BlockSpec(memory_space=pltpu.VMEM), anywhere),
        scratch_shapes=[
            vmem((2, 128, 32), BF16),
            vmem((128, 128), F32),
            vmem((48, 128), BF16),
            vmem((1, 64), F32),
            vmem((64, 512), BF16),
            vmem((64, 512), BF16),
            vmem((64, 512), BF16),
            vmem((64, 1024), BF16),
            vmem((64, 1024), BF16),
            vmem((1, 512), F32),
            vmem((1, 512), F32),
            vmem((1, 2048), F32),
            vmem((2, 1024, 64), BF16),
            vmem((2048, 256), BF16),
            vmem((256, 2048), BF16),
            vmem((4, 2, 256, 512), F32),
            vmem((4, 2, 48, 128), BF16),
            vmem((256, 1024), BF16),
            vmem((128, 1024), BF16),
            vmem((8, 16, 1024), BF16),
            vmem((4, 4, 1024), F32),
            vmem((4, 4, 1024), F32),
            vmem((16, 512), F32),
            vmem((4, 1024), F32),
            vmem((4, 1024), BF16),
            vmem((4, 4, 2, 4, 1024), BF16),
            vmem((64, 2048), F32),
            vmem((32, 128), BF16),
            vmem((8, 4, 32, 128), BF16),
            vmem((64, 256), F32),
            vmem((8, 4, 32, 128), BF16),
            vmem((8, 4, 32, 128), BF16),
            vmem((8, 32, 128), BF16),
            vmem((8, 32, 128), BF16),
            vmem((2, 32, 128), BF16),
            pltpu.SemaphoreType.DMA((SENDS,)),
            pltpu.SemaphoreType.DMA((SENDS,)),
            pltpu.SemaphoreType.DMA((32,)),
            pltpu.SemaphoreType.DMA((4, 2)),
        ],
        compiler_params=pltpu.CompilerParams(
            collective_id=0, has_side_effects=True, vmem_limit_bytes=48 * 1024 * 1024
        ),
        name="layer_step",
    )(
        tokens, state, mix_gain.reshape(1, -1), w_query, w_key, w_decay, w_value, w_gate,
        decay_offset.reshape(1, -1), head_gain.reshape(1, -1), w_out, mlp_gain.reshape(1, -1), w_up, w_down,
    )
    return mixed, new_state


def solution(mesh):
    in_specs = (
        P("dp", ("kv", "tp")),
        P(("dp", "kv"), "tp", None, None),
        P("kv"),
        P("kv", "tp"),
        P("kv", "tp"),
        P("kv", "tp"),
        P("kv", "tp"),
        P("kv", "tp"),
        P("tp"),
        P(),
        P("tp", "kv"),
        P(),
        P(None, ("kv", "tp")),
        P(("kv", "tp"), None),
    )
    out_specs = (P("dp", ("kv", "tp")), P(("dp", "kv"), "tp", None, None))
    return jax.shard_map(shards, mesh=mesh, in_specs=in_specs, out_specs=out_specs, check_vma=False)
```

```python
import jax
import jax.numpy as jnp
from jax import lax
from jax.experimental import pallas as pl
from jax.experimental.pallas import tpu as pltpu
from jax.sharding import PartitionSpec as P

MESH = pl.DeviceIdType.MESH
F32, BF16 = jnp.float32, jnp.bfloat16
D = 2048
EPS = 1e-06
NY, NZ = 4, 8
Q, K, R, S, V, G = (slice(0, 128), slice(128, 256), slice(256, 384), slice(384, 512), slice(512, 768), slice(768, 1024))
PIECES = ((V, (3,)), (G, (4,)), (slice(0, 256), (0, 1)), (slice(256, 512), (2,)))
COLUMNS = (Q, K, R, V, G)


def halves_side_by_side(top, bottom):
    lane = lax.broadcasted_iota(jnp.int32, top.shape, 1)
    return jnp.where(lane < 64, top, pltpu.roll(bottom, 64, 1))


def second_halves(top, bottom):
    lane = lax.broadcasted_iota(jnp.int32, top.shape, 1)
    return jnp.where(lane < 64, pltpu.roll(top, 64, 1), bottom)


def step(
    tok_h, state_h, gain_h, wq_h, wk_h, wd_h, wv_h, wg_h, off_h, hg_h, wo_h, mg_h, wu_h, wdn_h,
    mixed_ref, state,
    toks, unit, gain, wq, wk, wd, wv, wg, off, hg, mg, wo, wu, wdn,
    xg, wgat, zs, zr, ys, yr, cols, vals, gs, gr, gf, sp, sr, xf, fs, fr, fz, zr6, mx,
    send_sem, recv_sem, local_sem, gr_sem,
):
    kv, t = lax.axis_index("kv"), lax.axis_index("tp")
    y, z = lax.rem(kv, NY), lax.div(kv, NY)
    other = 1 - t

    def at_y(dy):
        return lax.rem(y + dy + NY, NY)

    def at_z(dz):
        return lax.rem(z + dz + NZ, NZ)

    barrier = pltpu.get_barrier_semaphore()

    def greet(to_y, to_z, to_t):
        pl.semaphore_signal(
            barrier, inc=1, device_id={"kv": to_z * NY + to_y, "tp": to_t}, device_id_type=MESH
        )

    greet(y, z, other)
    for dy in range(1, NY):
        greet(at_y(dy), z, t)
        greet(at_y(dy), z, other)
    for dz in range(1, NZ):
        greet(y, at_z(dz), t)
        greet(y, at_z(dz), other)
    greetings = 1 + 2 * (NY - 1) + 2 * (NZ - 1)

    local = []

    def fetch(src, dst):
        copy = pltpu.make_async_copy(src, dst, local_sem.at[len(local)])
        copy.start()
        local.append(copy)
        return copy

    sends = []

    def send(src, dst, to_y, to_z, to_t, recv=None):
        n = len(sends)
        copy = pltpu.make_async_remote_copy(
            src_ref=src,
            dst_ref=dst,
            send_sem=send_sem.at[n],
            recv_sem=recv_sem.at[n] if recv is None else recv,
            device_id={"kv": to_z * NY + to_y, "tp": to_t},
            device_id_type=MESH,
        )
        copy.start()
        sends.append(copy)
        return copy

    tok_in = [fetch(tok_h, toks.at[t]), fetch(gain_h, gain)]
    weights, staged = (wq_h, wk_h, wd_h, wv_h, wg_h), (wq, wk, wd, wv, wg)
    weight_in, own_in = [None] * 5, [None] * 5
    for n in (3, 4, 0, 1, 2):
        weight_in[n] = fetch(weights[n], staged[n])
    for n in (3, 4, 0, 1, 2):
        width = COLUMNS[n].stop - COLUMNS[n].start
        mine = pl.ds(pl.multiple_of(y * width, width), width)
        own_in[n] = fetch(
            weights[n].at[:, mine], wgat.at[pl.ds(pl.multiple_of(y * 64, 64), 64), COLUMNS[n]]
        )
    half_lanes = pl.ds(pl.multiple_of(t * 128, 128), 128)
    half_rows = pl.ds(pl.multiple_of(t * 128, 128), 128)
    wo_in = fetch(wo_h, wo.at[t])
    wu_in = fetch(wu_h, wu.at[:, half_lanes])
    wdn_in = fetch(wdn_h, wdn.at[half_rows])
    small_in = [fetch(off_h, off), fetch(hg_h, hg), fetch(mg_h, mg)]
    state_in = fetch(state_h, state)

    for copy in tok_in:
        copy.wait()
    tok = toks[t].astype(F32)
    both_gains = jnp.broadcast_to(gain[...], (128, 64)).T
    my_gain = jnp.where(t == 0, both_gains[:32], both_gains[32:])
    squares = jnp.sum(tok * tok, axis=0, keepdims=True)
    high = squares.astype(BF16).astype(F32)
    rows = lax.broadcasted_iota(jnp.int32, (16, 128), 0)
    sums = jnp.where(rows == 0, high, jnp.where(rows == 1, squares - high, 0.0))
    unit[0:32] = (tok * my_gain).astype(BF16)
    unit[32:48] = sums.astype(BF16)
    xg[y, t] = unit[...]
    for copy in weight_in:
        copy.wait()

    pl.semaphore_wait(barrier, greetings)

    x_in = [send(unit, xg.at[y, t], y, z, other)]
    for dy in range(1, NY):
        x_in.append(send(unit, xg.at[y, t], at_y(dy), z, t))
        x_in.append(send(unit, xg.at[y, t], at_y(dy), z, other))
    w_in = [[] for _ in range(5)]
    for n in (3, 4, 0, 1, 2):
        width = COLUMNS[n].stop - COLUMNS[n].start
        for dy in (2, 1, 3):
            theirs = pl.ds(pl.multiple_of(at_y(dy) * width, width), width)
            w_in[n].append(
                send(
                    staged[n].at[:, theirs],
                    wgat.at[pl.ds(pl.multiple_of(y * 64, 64), 64), COLUMNS[n]],
                    at_y(dy),
                    z,
                    t,
                )
            )
    wo_in.wait()
    wu_in.wait()
    wdn_in.wait()
    twin_in = [
        send(toks.at[t], toks.at[t], y, z, other),
        send(wo.at[t], wo.at[t], y, z, other),
        send(wu.at[:, half_lanes], wu.at[:, half_lanes], y, z, other),
        send(wdn.at[half_rows], wdn.at[half_rows], y, z, other),
    ]

    for copy in x_in:
        copy.wait_recv()
    blocks = [xg[a, b].astype(F32) for a in range(NY) for b in range(2)]
    x = jnp.concatenate([block[0:32] for block in blocks], axis=0).T.astype(BF16)
    row_squares = sum(block[32:33] + block[33:34] for block in blocks)
    spread = jnp.broadcast_to(row_squares, (128, 128)).T
    spread_high = spread.astype(BF16).astype(F32)
    lane = lax.broadcasted_iota(jnp.int32, (128, 128), 1)
    zs[:, S] = jnp.where(lane < 64, spread_high, spread - spread_high).astype(BF16)
    z_in = []
    for columns, members in PIECES:
        for n in members:
            own_in[n].wait()
            for copy in w_in[n]:
                copy.wait_recv()
        if members == (2,):
            zs[:, R] = jnp.dot(x, wgat[:, R], preferred_element_type=F32).astype(BF16)
        else:
            zs[:, columns] = jnp.dot(x, wgat[:, columns], preferred_element_type=F32).astype(BF16)
        z_in.append([])
        for dz in (4, 3, 5, 2, 6, 1, 7):
            theirs = pl.ds(pl.multiple_of(at_z(dz) * 16, 16), 16)
            z_in[-1].append(
                send(zs.at[theirs, columns], zr.at[z, :, columns], y, at_z(dz), t)
            )
    for (columns, members), copies in zip(PIECES, z_in):
        mine = pl.ds(pl.multiple_of(z * 16, 16), 16)
        total = zs[mine, columns].astype(F32)
        for copy in copies:
            copy.wait_recv()
        for dz in range(1, NZ):
            total = total + zr[at_z(dz), :, columns].astype(F32)
        for a in range(NY):
            ys[a, :, columns] = total[4 * a : 4 * a + 4]
    y_in = [send(ys.at[at_y(dy)], yr.at[y], at_y(dy), z, t) for dy in (2, 1, 3)]
    yr[y] = ys[y]
    for copy in small_in:
        copy.wait()
    state_in.wait()
    for copy in y_in:
        copy.wait_recv()

    got = [yr[a] for a in range(NY)]
    row_sum = got[0][:, 384:385] + got[0][:, 448:449]
    scale = lax.rsqrt(row_sum / D + EPS)
    queries = jnp.concatenate([g[:, Q] for g in got], axis=1) * scale * (256 ** -0.5)
    keys = jnp.concatenate([g[:, K] for g in got], axis=1) * scale
    retain = jax.nn.sigmoid(jnp.concatenate([g[:, R] for g in got], axis=1) * scale + off[...])
    cols[0:4] = queries
    cols[4:8] = keys
    cols[8:12] = retain
    cols[12:16] = jnp.zeros((4, 512), F32)
    upright = cols[...].T
    values = jnp.concatenate([g[:, V] for g in got], axis=1) * scale
    gates = jnp.concatenate([g[:, G] for g in got], axis=1) * scale
    silu = gates * jax.nn.sigmoid(gates)
    for b in range(4):
        for h in range(2):
            value = values[b : b + 1, h * 512 : h * 512 + 512]
            total = jnp.zeros((8, 512), F32)
            for i in range(0, 256, 32):
                at = slice(h * 256 + i, h * 256 + i + 32)
                fresh = (
                    upright[at, 8 + b : 9 + b] * state[b, h, i : i + 32, :]
                    + upright[at, 4 + b : 5 + b] * value
                )
                state[b, h, i : i + 32, :] = fresh
                part = upright[at, b : b + 1] * fresh
                total = total + ((part[0:8] + part[8:16]) + (part[16:24] + part[24:32]))
            readout = jnp.sum(total, axis=0, keepdims=True)
            power = jnp.mean(readout * readout, axis=1, keepdims=True)
            vals[b : b + 1, h * 512 : h * 512 + 512] = (
                readout * lax.rsqrt(power + EPS) * hg[...]
            )
    gs[...] = (vals[...] * silu).astype(BF16)

    low = lax.rem(z, 4)
    home = lax.div(z, 4)
    for dz in range(1, NZ):
        send(gs, gr.at[y, low, t], y, at_z(dz), home, gr_sem.at[low, t])
    n = len(sends)

    @pl.when(home != t)
    def _():
        pltpu.make_async_remote_copy(
            src_ref=gs, dst_ref=gr.at[y, low, t], send_sem=send_sem.at[n], recv_sem=gr_sem.at[low, t],
            device_id={"kv": kv, "tp": other}, device_id_type=MESH,
        ).start()

    @pl.when(home == t)
    def _():
        gr[y, low, t] = gs[...]

    twin_gs = pltpu.make_async_copy(gs, gs, send_sem.at[n])
    sends.append(None)
    g_in = []
    for a in range(4):
        for c in range(2):
            @pl.when(jnp.logical_or(z != 4 * t + a, t != c))
            def _():
                pltpu.make_async_copy(gs, gr.at[y, a, c], gr_sem.at[a, c]).wait()
        g_in.append([send(gr.at[y, a], gr.at[y, a], at_y(dy), z, t) for dy in (2, 1, 3)])
    for copies in g_in:
        for copy in copies:
            copy.wait_recv()
    for a in range(4):
        for yy in range(NY):
            for c in range(2):
                gf[16 * a + 4 * yy : 16 * a + 4 * yy + 4, 1024 * c : 1024 * c + 1024] = gr[yy, a, c].astype(F32)

    for copy in twin_in:
        copy.wait_recv()
    rows_of = (((1,), (1,)), ((), ()))
    branch = lax.dot_general(
        gf[:, 0:1024].astype(BF16), wo[0], rows_of, preferred_element_type=F32
    ) + lax.dot_general(gf[:, 1024:2048].astype(BF16), wo[1], rows_of, preferred_element_type=F32)
    both_tok = jnp.concatenate([toks[0].astype(F32), toks[1].astype(F32)], axis=0).T
    own_tok = jnp.where(t == 0, both_tok[0:64], both_tok[64:128])
    stream = (own_tok + branch).astype(BF16).astype(F32)
    packed = jnp.concatenate([stream[0:32], stream[32:64]], axis=1)
    sp[...] = packed.astype(BF16)
    s_in = {}
    for dz in (4, 3, 5, 2, 6, 1, 7):
        s_in[dz] = send(sp, sr.at[z, y], y, at_z(dz), t)
    sr[z, y] = sp[...]
    s_y = {}
    for dz in (0, 1, 7, 2, 6, 3, 5, 4):
        if dz:
            s_in[dz].wait_recv()
        src = at_z(-dz)
        s_y[dz] = [send(sr.at[src, y], sr.at[src, y], at_y(dy), z, t) for dy in (2, 1, 3)]
    hidden = jnp.zeros((64, 256), F32)
    power = jnp.zeros((64, 256), F32)
    for dz in (0, 1, 7, 2, 6, 3, 5, 4):
        src = at_z(-dz)
        for copy in s_y[dz]:
            copy.wait_recv()
        for p in range(2):
            a, b = sr[src, 2 * p].astype(F32), sr[src, 2 * p + 1].astype(F32)
            xf[0:32, 128 * p : 128 * p + 128] = halves_side_by_side(a, b)
            xf[32:64, 128 * p : 128 * p + 128] = second_halves(a, b)
        block = xf[...]
        power = power + block * block
        gain_here = mg[:, pl.ds(pl.multiple_of(src * 256, 256), 256)]
        hidden = hidden + jnp.dot(
            (block * gain_here).astype(BF16),
            wu[pl.ds(pl.multiple_of(src * 256, 256), 256), :],
            preferred_element_type=F32,
        )
    mlp_scale = lax.rsqrt(jnp.sum(power, axis=1, keepdims=True) / D + EPS)
    squared = jnp.square(jnp.maximum(hidden * mlp_scale, 0.0)).astype(BF16)

    order = (4, 3, 5, 2, 6, 1, 7, 0)
    d_in = {}
    for dz in order:
        theirs = pl.ds(pl.multiple_of(at_z(dz) * 256, 256), 256)
        part = jnp.dot(squared, wdn[:, theirs], preferred_element_type=F32)
        for p in range(2):
            top, bottom = part[0:32, 128 * p : 128 * p + 128], part[32:64, 128 * p : 128 * p + 128]
            fs[dz, 2 * p] = halves_side_by_side(top, bottom).astype(BF16)
            fs[dz, 2 * p + 1] = second_halves(top, bottom).astype(BF16)
        d_in[dz] = [send(fs.at[dz, at_y(dy)], fr.at[dz, dy], at_y(dy), z, t) for dy in (2, 1, 3)]
    e_in = []
    for dz in order:
        for copy in d_in[dz]:
            copy.wait_recv()
        total = fs[dz, y].astype(F32)
        for dy in range(1, NY):
            total = total + fr[dz, dy].astype(F32)
        if dz:
            fz[dz] = total.astype(BF16)
            e_in.append(send(fz.at[dz], zr6.at[dz], y, at_z(dz), t))
    for copy in e_in:
        copy.wait_recv()
    for dz in range(1, NZ):
        total = total + zr6[dz].astype(F32)
    mx[t] = (packed + total).astype(BF16)
    m_in = send(mx.at[t], mx.at[t], y, z, other)
    m_in.wait_recv()
    quarters = []
    for c in range(2):
        block = mx[c].astype(F32)
        quarters += [block, pltpu.roll(block, 64, 1)]
    upright = jnp.concatenate(quarters, axis=0).T
    mixed_ref[...] = jnp.where(t == 0, upright[0:32], upright[32:64]).astype(BF16)

    for copy in sends:
        if copy is not None:
            copy.wait_send()

    @pl.when(home != t)
    def _():
        twin_gs.wait()


def handed_on(mixed_in, new_in, mixed_ref, new_ref, sem):
    copies = [pltpu.make_async_copy(new_in.at[b], new_ref.at[b], sem.at[b]) for b in range(4)]
    copies.append(pltpu.make_async_copy(mixed_in, mixed_ref, sem.at[4]))
    for copy in copies:
        copy.start()
    for copy in copies:
        copy.wait()


SENDS = 7 + 15 + 4 + 28 + 3 + 8 + 12 + 7 + 24 + 24 + 7 + 1


def shards(tokens, state, mix_gain, w_query, w_key, w_decay, w_value, w_gate, decay_offset, head_gain, w_out, mlp_gain, w_up, w_down):
    anywhere = pl.BlockSpec(memory_space=pltpu.HBM)
    inside = pl.BlockSpec(memory_space=pltpu.VMEM)
    vmem = pltpu.VMEM
    mixed, new_state = pl.pallas_call(
        step,
        out_shape=(
            vmem(tokens.shape[::-1], BF16),
            vmem(state.shape, F32),
        ),
        in_specs=[anywhere] * 14,
        out_specs=(inside, inside),
        scratch_shapes=[
            vmem((2, 32, 128), BF16),
            vmem((48, 128), BF16),
            vmem((1, 64), F32),
            vmem((64, 512), BF16),
            vmem((64, 512), BF16),
            vmem((64, 512), BF16),
            vmem((64, 1024), BF16),
            vmem((64, 1024), BF16),
            vmem((1, 512), F32),
            vmem((1, 512), F32),
            vmem((1, 2048), F32),
            vmem((2, 64, 1024), BF16),
            vmem((2048, 256), BF16),
            vmem((256, 2048), BF16),
            vmem((4, 2, 48, 128), BF16),
            vmem((256, 1024), BF16),
            vmem((128, 1024), BF16),
            vmem((8, 16, 1024), BF16),
            vmem((4, 4, 1024), F32),
            vmem((4, 4, 1024), F32),
            vmem((16, 512), F32),
            vmem((4, 1024), F32),
            vmem((4, 1024), BF16),
            vmem((4, 4, 2, 4, 1024), BF16),
            vmem((64, 2048), F32),
            vmem((32, 128), BF16),
            vmem((8, 4, 32, 128), BF16),
            vmem((64, 256), F32),
            vmem((8, 4, 32, 128), BF16),
            vmem((8, 4, 32, 128), BF16),
            vmem((8, 32, 128), BF16),
            vmem((8, 32, 128), BF16),
            vmem((2, 32, 128), BF16),
            pltpu.SemaphoreType.DMA((SENDS,)),
            pltpu.SemaphoreType.DMA((SENDS,)),
            pltpu.SemaphoreType.DMA((32,)),
            pltpu.SemaphoreType.DMA((4, 2)),
        ],
        compiler_params=pltpu.CompilerParams(
            collective_id=0, has_side_effects=True, vmem_limit_bytes=62_500_000
        ),
        name="layer_step",
    )(
        tokens.T, state, mix_gain.reshape(1, -1), w_query, w_key, w_decay, w_value, w_gate,
        decay_offset.reshape(1, -1), head_gain.reshape(1, -1), w_out.T, mlp_gain.reshape(1, -1), w_up, w_down,
    )
    mixed, new_state = pl.pallas_call(
        handed_on,
        out_shape=(
            jax.ShapeDtypeStruct(mixed.shape, BF16),
            jax.ShapeDtypeStruct(state.shape, F32),
        ),
        in_specs=[inside] * 2,
        out_specs=(anywhere, anywhere),
        scratch_shapes=[pltpu.SemaphoreType.DMA((5,))],
        compiler_params=pltpu.CompilerParams(vmem_limit_bytes=1024 * 1024),
        name="handed_on",
    )(mixed, new_state)
    return mixed.T, new_state


def solution(mesh):
    in_specs = (
        P("dp", ("kv", "tp")),
        P(("dp", "kv"), "tp", None, None),
        P("kv"),
        P("kv", "tp"),
        P("kv", "tp"),
        P("kv", "tp"),
        P("kv", "tp"),
        P("kv", "tp"),
        P("tp"),
        P(),
        P("tp", "kv"),
        P(),
        P(None, ("kv", "tp")),
        P(("kv", "tp"), None),
    )
    out_specs = (P("dp", ("kv", "tp")), P(("dp", "kv"), "tp", None, None))
    return jax.shard_map(shards, mesh=mesh, in_specs=in_specs, out_specs=out_specs, check_vma=False)
```

```python
import jax
import jax.numpy as jnp
from jax import lax
from jax.experimental import pallas as pl
from jax.experimental.pallas import tpu as pltpu
from jax.sharding import PartitionSpec as P

MESH = pl.DeviceIdType.MESH
F32, BF16 = jnp.float32, jnp.bfloat16
D = 2048
EPS = 1e-06
NX, NY, NZ = 4, 4, 8
Q, K, R, S, V, G = (slice(0, 128), slice(128, 256), slice(256, 384), slice(384, 512), slice(512, 768), slice(768, 1024))
PIECES = ((V, (3,)), (G, (4,)), (slice(0, 256), (0, 1)), (slice(256, 512), (2,)))
COLUMNS = (Q, K, R, V, G)


def halves_side_by_side(top, bottom):
    lane = lax.broadcasted_iota(jnp.int32, top.shape, 1)
    return jnp.where(lane < 64, top, pltpu.roll(bottom, 64, 1))


def second_halves(top, bottom):
    lane = lax.broadcasted_iota(jnp.int32, top.shape, 1)
    return jnp.where(lane < 64, pltpu.roll(top, 64, 1), bottom)


def slotted(rows, t):
    parts = rows.reshape(8, 1, 8, rows.shape[1])
    pair = [jnp.where(t == c, parts, 0.0) for c in range(2)]
    return jnp.concatenate(pair, axis=1).reshape(128, rows.shape[1])


def step(
    tok_h, state_h, gain_h, wq_h, wk_h, wd_h, wv_h, wg_h, off_h, hg_h, wo_h, mg_h, wu_h, wdn_h,
    mixed_ref, state,
    toks, unit, gain, wq, wk, wd, wv, wg, off, hg, mg, wo, wu, wdn,
    xg, wgat, zs, zr, ys, yr, cols, upright, vals, outs, gs, gr, gf, tokt, sp, sr, xf, wdt, part, fs, fr, fz, zr6, tw,
    send_sem, recv_sem, local_sem, gr_sem,
):
    kv, t = lax.axis_index("kv"), lax.axis_index("tp")
    y, z = lax.rem(kv, NY), lax.div(kv, NY)
    x = lax.axis_index("dp")
    other = 1 - t

    def at_x(dx):
        return lax.rem(x + dx, NX)

    def at_y(dy):
        return lax.rem(y + dy + NY, NY)

    def at_z(dz):
        return lax.rem(z + dz + NZ, NZ)

    barrier = pltpu.get_barrier_semaphore()

    def greet(to_y, to_z, to_t):
        pl.semaphore_signal(
            barrier, inc=1, device_id={"kv": to_z * NY + to_y, "tp": to_t}, device_id_type=MESH
        )

    greet(y, z, other)
    for dy in range(1, NY):
        greet(at_y(dy), z, t)
        greet(at_y(dy), z, other)
    for dz in range(1, NZ):
        greet(y, at_z(dz), t)
        greet(y, at_z(dz), other)
    for dx in range(1, NX):
        pl.semaphore_signal(barrier, inc=1, device_id={"dp": at_x(dx)}, device_id_type=MESH)
    greetings = 1 + 2 * (NY - 1) + 2 * (NZ - 1) + (NX - 1)

    local = []

    def fetch(src, dst):
        copy = pltpu.make_async_copy(src, dst, local_sem.at[len(local)])
        copy.start()
        local.append(copy)
        return copy

    sends = []

    def send(src, dst, to_y, to_z, to_t, recv=None, to_x=None):
        n = len(sends)
        to = {"kv": to_z * NY + to_y, "tp": to_t} if to_x is None else {"dp": to_x}
        copy = pltpu.make_async_remote_copy(
            src_ref=src,
            dst_ref=dst,
            send_sem=send_sem.at[n],
            recv_sem=recv_sem.at[n] if recv is None else recv,
            device_id=to,
            device_id_type=MESH,
        )
        copy.start()
        sends.append(copy)
        return copy

    drained = []

    def drain():
        for copy in sends[len(drained) :]:
            if copy is not None:
                copy.wait_send()
            drained.append(copy)

    tok_in = [fetch(tok_h, toks.at[t, z]), fetch(gain_h, gain)]
    weights, staged = (wq_h, wk_h, wd_h, wv_h, wg_h), (wq, wk, wd, wv, wg)
    weight_in, own_in = [None] * 5, [None] * 5
    for n in (3, 4, 0, 1, 2):
        weight_in[n] = fetch(weights[n], staged[n])
    for n in (3, 4, 0, 1, 2):
        width = COLUMNS[n].stop - COLUMNS[n].start
        mine = pl.ds(pl.multiple_of(y * width, width), width)
        own_in[n] = fetch(
            weights[n].at[:, mine], wgat.at[pl.ds(pl.multiple_of(y * 64, 64), 64), COLUMNS[n]]
        )
    half_lanes = pl.ds(pl.multiple_of(t * 128, 128), 128)
    half_rows = pl.ds(pl.multiple_of(t * 128, 128), 128)
    wo_in = fetch(wo_h, wo.at[t, z])
    wu_in = fetch(wu_h, wu.at[:, half_lanes])
    wdn_in = fetch(wdn_h, wdn.at[half_rows])
    small_in = [fetch(off_h, off), fetch(hg_h, hg), fetch(mg_h, mg)]
    state_in = fetch(state_h, state)

    for copy in tok_in:
        copy.wait()
    tok = toks[t, z].astype(F32)
    both_gains = jnp.broadcast_to(gain[...], (128, 64)).T
    my_gain = jnp.where(t == 0, both_gains[:32], both_gains[32:])
    squares = jnp.sum(tok * tok, axis=0, keepdims=True)
    high = squares.astype(BF16).astype(F32)
    rows = lax.broadcasted_iota(jnp.int32, (16, 128), 0)
    sums = jnp.where(rows == 0, high, jnp.where(rows == 1, squares - high, 0.0))
    unit[0:32] = (tok * my_gain).astype(BF16)
    unit[32:48] = sums.astype(BF16)
    xg[y, t] = unit[...]
    for copy in weight_in:
        copy.wait()

    pl.semaphore_wait(barrier, greetings)

    x_in = [send(unit, xg.at[y, t], y, z, other)]
    for dy in range(1, NY):
        x_in.append(send(unit, xg.at[y, t], at_y(dy), z, t))
        x_in.append(send(unit, xg.at[y, t], at_y(dy), z, other))
    w_in = [[] for _ in range(5)]
    for n in (3, 4, 0, 1, 2):
        width = COLUMNS[n].stop - COLUMNS[n].start
        for dy in (2, 1, 3):
            theirs = pl.ds(pl.multiple_of(at_y(dy) * width, width), width)
            w_in[n].append(
                send(
                    staged[n].at[:, theirs],
                    wgat.at[pl.ds(pl.multiple_of(y * 64, 64), 64), COLUMNS[n]],
                    at_y(dy),
                    z,
                    t,
                )
            )
    wo_in.wait()
    quarter = pl.ds(pl.multiple_of(x * 16, 16), 16)
    o_in = {}
    for dz in (1, 7, 2, 6, 3, 5, 4):
        o_in[dz] = send(wo.at[t, z, quarter], wo.at[t, z, quarter], y, at_z(dz), t)
    wu_in.wait()
    wdn_in.wait()
    twin_in = [
        send(wu.at[:, half_lanes], wu.at[:, half_lanes], y, z, other),
        send(wdn.at[half_rows], wdn.at[half_rows], y, z, other),
    ]
    q_in = []

    def hand_on(*hops):
        for dz in hops:
            o_in[dz].wait_recv()
            held = wo.at[t, at_z(-dz), quarter]
            for dx in (2, 1, 3):
                q_in.append(send(held, held, y, z, t, to_x=at_x(dx)))

    rows_of = (((1,), (1,)), ((), ()))
    for copy in x_in:
        copy.wait_recv()
    blocks = [xg[a, b].astype(F32) for a in range(NY) for b in range(2)]
    scaled = jnp.concatenate([block[0:32] for block in blocks], axis=0).T.astype(BF16)
    row_squares = sum(block[32:33] + block[33:34] for block in blocks)
    spread = jnp.broadcast_to(row_squares, (128, 128)).T
    spread_high = spread.astype(BF16).astype(F32)
    lane = lax.broadcasted_iota(jnp.int32, (128, 128), 1)
    zs[:, S] = jnp.where(lane < 64, spread_high, spread - spread_high).astype(BF16)
    hand_on(1, 7)
    z_in = []
    for columns, members in PIECES:
        for n in members:
            own_in[n].wait()
            for copy in w_in[n]:
                copy.wait_recv()
        if members == (2,):
            zs[:, R] = jnp.dot(scaled, wgat[:, R], preferred_element_type=F32).astype(BF16)
        else:
            zs[:, columns] = jnp.dot(scaled, wgat[:, columns], preferred_element_type=F32).astype(BF16)
        z_in.append([])
        for dz in (4, 3, 5, 2, 6, 1, 7):
            theirs = pl.ds(pl.multiple_of(at_z(dz) * 16, 16), 16)
            z_in[-1].append(
                send(zs.at[theirs, columns], zr.at[z, :, columns], y, at_z(dz), t)
            )
        if members == (3,):
            hand_on(2, 6)
    k_in = [send(toks.at[t, z], toks.at[t, z], y, at_z(dz), t) for dz in (4, 3, 5, 2, 6, 1, 7)]
    hand_on(3, 5, 4)
    for copy in twin_in:
        copy.wait_recv()
    for at in range(0, 2048, 256):
        wdt[at : at + 256] = wdn[:, at : at + 256].astype(F32).T.astype(BF16)
    for (columns, members), copies in zip(PIECES, z_in):
        mine = pl.ds(pl.multiple_of(z * 16, 16), 16)
        total = zs[mine, columns].astype(F32)
        for copy in copies:
            copy.wait_recv()
        for dz in range(1, NZ):
            total = total + zr[at_z(dz), :, columns].astype(F32)
        for a in range(NY):
            ys[a, :, columns] = total[4 * a : 4 * a + 4]
    y_in = [send(ys.at[at_y(dy)], yr.at[y], at_y(dy), z, t) for dy in (2, 1, 3)]
    yr[y] = ys[y]
    for copy in k_in + q_in:
        copy.wait_recv()
    twin_in = [
        send(wo.at[t], wo.at[t], y, z, other),
        send(toks.at[t], toks.at[t], y, z, other),
    ]
    for copy in small_in:
        copy.wait()
    state_in.wait()
    for copy in y_in:
        copy.wait_recv()

    got = [yr[a] for a in range(NY)]
    row_sum = got[0][:, 384:385] + got[0][:, 448:449]
    scale = lax.rsqrt(row_sum / D + EPS)
    queries = jnp.concatenate([g[:, Q] for g in got], axis=1) * scale * (256 ** -0.5)
    keys = jnp.concatenate([g[:, K] for g in got], axis=1) * scale
    retain = jax.nn.sigmoid(jnp.concatenate([g[:, R] for g in got], axis=1) * scale + off[...])
    cols[0:4] = queries * retain
    cols[4:8] = keys
    cols[8:12] = retain
    cols[12:16] = jnp.zeros((4, 512), F32)
    upright[...] = cols[...].T
    matches = queries * keys
    values = jnp.concatenate([g[:, V] for g in got], axis=1) * scale
    vals[...] = values
    gates = jnp.concatenate([g[:, G] for g in got], axis=1) * scale
    silu = gates * jax.nn.sigmoid(gates)
    for b in range(4):
        for h in range(2):
            total = jnp.zeros((8, 512), F32)
            for i in range(0, 256, 32):
                at = slice(h * 256 + i, h * 256 + i + 32)
                term = upright[at, b : b + 1] * state[b, h, i : i + 32, :]
                total = total + ((term[0:8] + term[8:16]) + (term[16:24] + term[24:32]))
            match = jnp.sum(matches[b : b + 1, h * 256 : h * 256 + 256], axis=1, keepdims=True)
            readout = (
                jnp.sum(total, axis=0, keepdims=True)
                + match * values[b : b + 1, h * 512 : h * 512 + 512]
            )
            power = jnp.mean(readout * readout, axis=1, keepdims=True)
            outs[b : b + 1, h * 512 : h * 512 + 512] = (
                readout * lax.rsqrt(power + EPS) * hg[...]
            )
    gs[...] = (outs[...] * silu).astype(BF16)

    low = lax.rem(y, 2)
    home = lax.div(y, 2)
    for dy in (2, 1, 3):
        send(gs, gr.at[low, t], at_y(dy), z, home, gr_sem.at[low, t])
    n = len(sends)

    @pl.when(home != t)
    def _():
        pltpu.make_async_remote_copy(
            src_ref=gs, dst_ref=gr.at[low, t], send_sem=send_sem.at[n], recv_sem=gr_sem.at[low, t],
            device_id={"kv": kv, "tp": other}, device_id_type=MESH,
        ).start()

    @pl.when(home == t)
    def _():
        gr[low, t] = gs[...]

    twin_gs = pltpu.make_async_copy(gs, gs, send_sem.at[n])
    sends.append(None)
    for b in range(4):
        for h in range(2):
            value = vals[b : b + 1, h * 512 : h * 512 + 512]
            for i in range(0, 256, 32):
                at = slice(h * 256 + i, h * 256 + i + 32)
                state[b, h, i : i + 32, :] = (
                    upright[at, 8 + b : 9 + b] * state[b, h, i : i + 32, :]
                    + upright[at, 4 + b : 5 + b] * value
                )
    drain()

    @pl.when(home != t)
    def _():
        twin_gs.wait()

    for copy in twin_in:
        copy.wait_recv()
    for p in range(4):
        own = jnp.concatenate([toks[c % 2, 2 * p + c // 2].astype(F32) for c in range(4)], axis=0)
        tokt[:, 128 * p : 128 * p + 128] = own.T
    here = pl.ds(pl.multiple_of(z * 16 + t * 8, 8), 8)
    own_tok = tokt[here]
    for a in range(2):
        for c in range(2):
            @pl.when(jnp.logical_or(y != 2 * t + a, t != c))
            def _():
                pltpu.make_async_copy(gs, gr.at[a, c], gr_sem.at[a, c]).wait()

            gf[4 * a : 4 * a + 4, 1024 * c : 1024 * c + 1024] = gr[a, c].astype(F32)

    gb = gf[...].astype(BF16)
    branch = sum(
        lax.dot_general(
            wo[c].reshape(512, 1024), gb[:, 1024 * c : 1024 * c + 1024], rows_of,
            preferred_element_type=F32,
        )
        for c in range(2)
    ).T
    sp[...] = (own_tok + branch).astype(BF16)
    s_in = {}
    for dz in (4, 3, 5, 2, 6, 1, 7):
        s_in[dz] = send(sp, sr.at[z, y], y, at_z(dz), t)
    sr[z, y] = sp[...]
    s_y = {}
    for dz in (0, 1, 7, 2, 6, 3, 5, 4):
        if dz:
            s_in[dz].wait_recv()
        src = at_z(-dz)
        s_y[dz] = [send(sr.at[src, y], sr.at[src, y], at_y(dy), z, t) for dy in (2, 1, 3)]
    drain()
    for dz in (0, 1, 7, 2, 6, 3, 5, 4):
        src = at_z(-dz)
        for copy in s_y[dz]:
            copy.wait_recv()
        rows = pl.ds(pl.multiple_of(src * 8, 8), 8)
        for p in range(2):
            for m in range(4):
                a = sr[src, 2 * p, :, 128 * m : 128 * m + 128].astype(F32)
                b = sr[src, 2 * p + 1, :, 128 * m : 128 * m + 128].astype(F32)
                at = 512 * m + 128 * p
                xf[rows, at : at + 128] = halves_side_by_side(a, b)
                xf[rows, at + 256 : at + 384] = second_halves(a, b)
    block = xf[...]
    power = jnp.sum(block * block, axis=1, keepdims=True)
    hidden = jnp.dot((block * mg[...]).astype(BF16), wu[...], preferred_element_type=F32)
    mlp_scale = lax.rsqrt(power / D + EPS)
    squared = slotted(jnp.square(jnp.maximum(hidden * mlp_scale, 0.0)), t).astype(BF16)
    near = pl.ds(pl.multiple_of(z * 256 + lax.div(y, 2) * 128, 128), 128)
    turned = slotted(xf[:, near], t).T
    turned = jnp.where(lax.rem(y, 2) == 0, turned[0:64], turned[64:128])
    own_stream = jnp.stack(
        [turned[c : c + 16] + pltpu.roll(turned[c + 16 : c + 32], 8, 1) for c in (0, 32)]
    )

    order = (4, 3, 5, 2, 6, 1, 7, 0)
    d_in = {}
    for dz in order:
        theirs = pl.ds(pl.multiple_of(at_z(dz) * 256, 256), 256)
        part[...] = lax.dot_general(wdt[theirs], squared, rows_of, preferred_element_type=F32)
        for a in range(NY):
            for c in range(2):
                at = 64 * a + 32 * c
                fs[dz, a, c] = (
                    part[at : at + 16] + pltpu.roll(part[at + 16 : at + 32], 8, 1)
                ).astype(BF16)
        d_in[dz] = [send(fs.at[dz, at_y(dy)], fr.at[dz, dy], at_y(dy), z, t) for dy in (2, 1, 3)]
    e_in = []
    for dz in order:
        for copy in d_in[dz]:
            copy.wait_recv()
        total = fs[dz, y].astype(F32)
        for dy in range(1, NY):
            total = total + fr[dz, dy].astype(F32)
        if dz:
            fz[dz] = total.astype(BF16)
            for c in (t, other):
                e_in.append(send(fz.at[dz, c], zr6.at[dz, t], y, at_z(dz), c))
    total = total + own_stream
    mine = jnp.where(t == 0, total[0], total[1])
    tw[0] = jnp.where(t == 0, total[1], total[0])
    tw_in = send(tw.at[0], tw.at[1], y, z, other)
    drain()
    for copy in e_in:
        copy.wait_recv()
    tw_in.wait_recv()
    theirs = tw[1]
    halves = [jnp.where(t == 0, mine, theirs), jnp.where(t == 0, theirs, mine)]
    for dz in range(1, NZ):
        halves = [halves[c] + zr6[dz, c].astype(F32) for c in range(2)]
    lane = lax.broadcasted_iota(jnp.int32, (16, 128), 1)
    first = lax.rem(lane, 16) < 8
    mixed_ref[0:16] = jnp.where(first, halves[0], halves[1]).astype(BF16)
    back = [pltpu.roll(half, 120, 1) for half in halves]
    mixed_ref[16:32] = jnp.where(first, back[0], back[1]).astype(BF16)
    drain()


def handed_on(mixed_in, new_in, mixed_ref, new_ref, sem):
    copies = [pltpu.make_async_copy(new_in.at[b], new_ref.at[b], sem.at[b]) for b in range(4)]
    copies.append(pltpu.make_async_copy(mixed_in, mixed_ref, sem.at[4]))
    for copy in copies:
        copy.start()
    for copy in copies:
        copy.wait()


SENDS = 7 + 15 + 7 + 2 + 21 + 28 + 7 + 3 + 2 + 4 + 7 + 24 + 24 + 14 + 1


def shards(tokens, state, mix_gain, w_query, w_key, w_decay, w_value, w_gate, decay_offset, head_gain, w_out, mlp_gain, w_up, w_down):
    anywhere = pl.BlockSpec(memory_space=pltpu.HBM)
    inside = pl.BlockSpec(memory_space=pltpu.VMEM)
    vmem = pltpu.VMEM
    mixed, new_state = pl.pallas_call(
        step,
        out_shape=(
            vmem(tokens.shape[::-1], BF16),
            vmem(state.shape, F32),
        ),
        in_specs=[anywhere] * 14,
        out_specs=(inside, inside),
        scratch_shapes=[
            vmem((2, 8, 32, 128), BF16),
            vmem((48, 128), BF16),
            vmem((1, 64), F32),
            vmem((64, 512), BF16),
            vmem((64, 512), BF16),
            vmem((64, 512), BF16),
            vmem((64, 1024), BF16),
            vmem((64, 1024), BF16),
            vmem((1, 512), F32),
            vmem((1, 512), F32),
            vmem((1, 2048), F32),
            vmem((2, 8, 64, 1024), BF16),
            vmem((2048, 256), BF16),
            vmem((256, 2048), BF16),
            vmem((4, 2, 48, 128), BF16),
            vmem((256, 1024), BF16),
            vmem((128, 1024), BF16),
            vmem((8, 16, 1024), BF16),
            vmem((4, 4, 1024), F32),
            vmem((4, 4, 1024), F32),
            vmem((16, 512), F32),
            vmem((512, 16), F32),
            vmem((4, 1024), F32),
            vmem((4, 1024), F32),
            vmem((4, 1024), BF16),
            vmem((2, 2, 4, 1024), BF16),
            vmem((8, 2048), F32),
            vmem((128, 512), F32),
            vmem((8, 512), BF16),
            vmem((8, 4, 8, 512), BF16),
            vmem((64, 2048), F32),
            vmem((2048, 256), BF16),
            vmem((256, 128), F32),
            vmem((8, 4, 2, 16, 128), BF16),
            vmem((8, 4, 2, 16, 128), BF16),
            vmem((8, 2, 16, 128), BF16),
            vmem((8, 2, 16, 128), BF16),
            vmem((2, 16, 128), F32),
            pltpu.SemaphoreType.DMA((SENDS,)),
            pltpu.SemaphoreType.DMA((SENDS,)),
            pltpu.SemaphoreType.DMA((32,)),
            pltpu.SemaphoreType.DMA((2, 2)),
        ],
        compiler_params=pltpu.CompilerParams(
            collective_id=0, has_side_effects=True, vmem_limit_bytes=62_500_000
        ),
        name="layer_step",
    )(
        tokens.T, state, mix_gain.reshape(1, -1), w_query, w_key, w_decay, w_value, w_gate,
        decay_offset.reshape(1, -1), head_gain.reshape(1, -1), w_out.T, mlp_gain.reshape(1, -1), w_up, w_down,
    )
    mixed, new_state = pl.pallas_call(
        handed_on,
        out_shape=(
            jax.ShapeDtypeStruct(mixed.shape, BF16),
            jax.ShapeDtypeStruct(state.shape, F32),
        ),
        in_specs=[inside] * 2,
        out_specs=(anywhere, anywhere),
        scratch_shapes=[pltpu.SemaphoreType.DMA((5,))],
        compiler_params=pltpu.CompilerParams(vmem_limit_bytes=1024 * 1024),
        name="handed_on",
    )(mixed, new_state)
    return mixed.T, new_state


def solution(mesh):
    in_specs = (
        P("dp", ("kv", "tp")),
        P(("dp", "kv"), "tp", None, None),
        P("kv"),
        P("kv", "tp"),
        P("kv", "tp"),
        P("kv", "tp"),
        P("kv", "tp"),
        P("kv", "tp"),
        P("tp"),
        P(),
        P("tp", "kv"),
        P(),
        P(None, ("kv", "tp")),
        P(("kv", "tp"), None),
    )
    out_specs = (P("dp", ("kv", "tp")), P(("dp", "kv"), "tp", None, None))
    return jax.shard_map(shards, mesh=mesh, in_specs=in_specs, out_specs=out_specs, check_vma=False)
```
